32 devices in a mesh: grp: 2 (over y), sp: 4 (over z), tp: 4 (over x, core).
Axes of the slice: x: 2, y: 2, z: 4, core: 2. Of those that a mesh axis runs over, the one named last changes fastest.
Arguments:
- query_a: bfloat16 [3072, 1024], P(('grp', 'sp'), 'tp'), parts along dimension 0, may hold values from -6 to 6
- key_a: bfloat16 [3072, 1024], P(('grp', 'sp'), 'tp'), parts along dimension 0, may hold values from -6 to 6
- query_b: bfloat16 [3072, 512], P(('grp', 'sp'), 'tp'), parts along dimension 0, may hold values from -6 to 6
- key_b: bfloat16 [3072, 512], P(('grp', 'sp'), 'tp'), parts along dimension 0, may hold values from -6 to 6
- values_a: bfloat16 [3072, 2048], P(('grp', 'sp'), 'tp'), parts along dimension 0, may hold values from -6 to 6
- values_b: bfloat16 [3072, 2048], P(('grp', 'sp'), 'tp'), parts along dimension 0, may hold values from -6 to 6
- outgate_a: bfloat16 [3072, 2048], P(('grp', 'sp'), 'tp'), parts along dimension 0, may hold values from -8 to 8
- outgate_b: bfloat16 [3072, 2048], P(('grp', 'sp'), 'tp'), parts along dimension 0, may hold values from -8 to 8
- input_pre: float32 [2, 8, 3072], P(None, 'tp', ('grp', 'sp')), parts along dimension 2, may hold values from -8 to 110, as said below
- forget_pre: float32 [2, 8, 3072], P(None, 'tp', ('grp', 'sp')), parts along dimension 2, may hold values from -4 to 16
- resid: bfloat16 [3072, 2048], P(('grp', 'sp', 'tp')), parts along dimension 0, may hold values from -6 to 6
- out_proj: bfloat16 [2048, 2, 2048], P(None, None, 'tp'), may hold values from -0.1875 to 0.1875
- norm_gain: float32 [2048], replicated, may hold values from 0.1 to 1.9
- w_gate: bfloat16 [2048, 5120], P('sp', 'tp'), may hold values from -0.125 to 0.125
- w_up: bfloat16 [2048, 5120], P('sp', 'tp'), may hold values from -0.125 to 0.125
- w_down: bfloat16 [2048, 5120], P('sp', 'tp'), may hold values from -0.078125 to 0.078125
Outputs:
- mixed: bfloat16 [3072, 2048], P(('grp', 'sp', 'tp')), parts along dimension 0
The draws below stay inside these ranges and needn't reach their ends.
There are 2 independent parts, one for each index of `grp`. The reference program is written for one: setup_inputs(seed, part) draws one part's arguments, and reference() takes and returns one part's arrays. A program takes and returns all parts, laid end to end along the dimension named above; an argument that names none is the same for every part. Nothing has to cross between parts.
Inputs may be any that keep to these rules, and one draw needn't show every extreme that they name: `input_pre`: pre-activations of the exponential input gate.
All inputs are finite; a program needn't handle non-finite values.
Results may differ from the reference program's by a relative error of at most 0.014.
Values may be sent and summed in bfloat16 or wider, within the bound.
A program may use at most 64 MiB of HBM per device.

```python
import math
import jax
import jax.numpy as jnp
from jax import lax

D = 2048
FF = 5120
GROUP_HEADS = 8
DKA = 128
DKB = 64
DV = 256
TOK_DEV = 384
SEQUENCE_LENGTH = 1536
N_TP = 4


def draw_input_pre(key, part):
    complete_shape = (2, GROUP_HEADS, SEQUENCE_LENGTH)
    value_rows = 1.2 * jax.random.normal(jax.random.fold_in(key, 16), complete_shape, jnp.float32)
    return jnp.clip(value_rows, -8.0, 110.0)


def draw_forget_pre(key, part):
    complete_shape = (2, GROUP_HEADS, SEQUENCE_LENGTH)
    block_count = SEQUENCE_LENGTH // TOK_DEV
    fast_share = 0.5
    quick_head = jax.random.uniform(jax.random.fold_in(key, 21), (2, GROUP_HEADS, 1), jnp.float32) < fast_share
    keep_ratio = jnp.exp(jax.random.uniform(jax.random.fold_in(key, 22), (2, GROUP_HEADS, 1), jnp.float32, math.log(0.15), math.log(0.7)))
    slow_base = jnp.log(SEQUENCE_LENGTH / keep_ratio)
    fast_base = jax.random.uniform(jax.random.fold_in(key, 23), (2, GROUP_HEADS, 1), jnp.float32, 2.5, 4.0)
    offsets = jax.random.uniform(jax.random.fold_in(key, 24), (2, GROUP_HEADS, block_count, 1), jnp.float32, -0.7, 0.7)
    offsets = jnp.broadcast_to(offsets, (2, GROUP_HEADS, block_count, TOK_DEV)).reshape(complete_shape)
    jitter = jnp.clip(0.6 * jax.random.normal(jax.random.fold_in(key, 26), complete_shape, jnp.float32), -1.8, 1.8)
    spike_entries = jax.random.randint(jax.random.fold_in(key, 27), (2, GROUP_HEADS, 2, 1), 0, SEQUENCE_LENGTH)
    spike_position = jnp.any(jnp.arange(SEQUENCE_LENGTH)[None, None, None, :] == spike_entries, axis=2)
    spike_magnitude = jax.random.uniform(jax.random.fold_in(key, 28), complete_shape, jnp.float32, 0.0, 1.4)
    value_rows = jnp.where(quick_head, fast_base, slow_base) + offsets + jitter
    value_rows = jnp.where(jnp.logical_and(spike_position, jnp.logical_not(quick_head)), spike_magnitude, value_rows)
    return jnp.clip(value_rows, -4.0, 16.0)


def steps_of(stream_key, dims, pieces, least, top_value):
    gain = 1.0
    for dim, shards_of in pieces:
        steps = jax.random.uniform(jax.random.fold_in(jax.random.fold_in(stream_key, 6), dim), (shards_of,), jnp.float32, least / len(pieces), top_value / len(pieces))
        gain = gain * jnp.repeat(jnp.exp(steps), dims[dim] // shards_of).reshape((-1,) + (1,) * (len(dims) - 1 - dim))
    return gain


def noise(key, dims, scale, reach, shards=(), held_as=jnp.bfloat16):
    values = scale * jax.random.normal(key, dims, jnp.float32)
    if shards:
        values = values * steps_of(key, dims, shards, -0.22, 0.18)
    return jnp.clip(values, -reach, reach).astype(held_as)


def setup_inputs(seed: int = 0, part: int = 0) -> dict:
    key_of = jax.random.split(jax.random.key(seed), 17)
    part_splits = jax.random.split(jax.random.fold_in(key_of[16], part), 17)
    query_a = noise(part_splits[0], (SEQUENCE_LENGTH, GROUP_HEADS * DKA), 1.0, 6.0, ((0, 4), (1, 4)))
    key_a = noise(part_splits[1], (SEQUENCE_LENGTH, GROUP_HEADS * DKA), 1.0, 6.0, ((0, 4), (1, 4)))
    query_b = noise(part_splits[2], (SEQUENCE_LENGTH, GROUP_HEADS * DKB), 1.0, 6.0, ((0, 4), (1, 4)))
    key_b = noise(part_splits[3], (SEQUENCE_LENGTH, GROUP_HEADS * DKB), 1.0, 6.0, ((0, 4), (1, 4)))
    values_a = noise(part_splits[4], (SEQUENCE_LENGTH, GROUP_HEADS * DV), 1.0, 6.0, ((0, 4), (1, 4)))
    values_b = noise(part_splits[5], (SEQUENCE_LENGTH, GROUP_HEADS * DV), 1.0, 6.0, ((0, 4), (1, 4)))
    outgate_a = noise(part_splits[6], (SEQUENCE_LENGTH, GROUP_HEADS * DV), 1.5, 8.0, ((0, 4), (1, 4)))
    outgate_b = noise(part_splits[7], (SEQUENCE_LENGTH, GROUP_HEADS * DV), 1.5, 8.0, ((0, 4), (1, 4)))
    input_pre = draw_input_pre(jax.random.fold_in(jax.random.fold_in(key_of[16], part), 71), part)
    forget_pre = draw_forget_pre(jax.random.fold_in(jax.random.fold_in(key_of[16], part), 71), part)
    resid = noise(part_splits[10], (SEQUENCE_LENGTH, D), 1.0, 6.0, ((0, 16),))
    out_proj = noise(key_of[11], (D, 2, GROUP_HEADS * DV), (GROUP_HEADS * DV // 2) ** -0.5, 0.1875, ((2, 4),))
    norm_gain = jnp.clip(1.0 + 0.18 * jax.random.normal(key_of[12], (D,), jnp.float32), 0.1, 1.9)
    w_gate = noise(key_of[13], (D, FF), D ** -0.5, 0.125, ((0, 4), (1, 4)))
    w_up = noise(key_of[14], (D, FF), D ** -0.5, 0.125, ((0, 4), (1, 4)))
    w_down = noise(key_of[15], (D, FF), FF ** -0.5, 0.078125, ((0, 4), (1, 4)))
    return {"query_a": query_a, "key_a": key_a, "query_b": query_b, "key_b": key_b, "values_a": values_a, "values_b": values_b, "outgate_a": outgate_a, "outgate_b": outgate_b, "input_pre": input_pre, "forget_pre": forget_pre, "resid": resid, "out_proj": out_proj, "norm_gain": norm_gain, "w_gate": w_gate, "w_up": w_up, "w_down": w_down}


EPS = 1e-06
NEG = -1e+30

def summarize(key_heads, value_head_rows, input_log, forget_raw):
    cum_forget = jnp.cumsum(jax.nn.log_sigmoid(forget_raw), axis=1)
    offset_log = input_log - cum_forget
    block_sum = cum_forget[:, -1]
    block_max = block_sum + lax.optimization_barrier(jnp.max(offset_log, axis=1))
    key_decay = jnp.exp(block_sum[:, None] + offset_log - block_max[:, None])
    scaled_keys = (key_heads.astype(jnp.float32) * jnp.transpose(key_decay)[:, :, None]).astype(jnp.bfloat16)
    block_memory_state = jnp.einsum('eif,eiw->ifw', scaled_keys.astype(jnp.float32), value_head_rows.astype(jnp.float32))
    return (block_memory_state, block_max, block_sum, offset_log)

def head_outputs(query_head_rows, key_heads, value_head_rows, outgate, offset_log, carried_over, mstate, key_width):
    length = query_head_rows.shape[0]
    run_max = jnp.maximum(lax.cummax(offset_log, axis=1), mstate[:, None])
    causal = jnp.arange(length)[:, None] >= jnp.arange(length)[None, :]
    exponent = jnp.where(causal[None], offset_log[:, None, :] - run_max[:, :, None], -jnp.inf)
    scores = jnp.einsum('thk,shk->hts', query_head_rows.astype(jnp.float32), key_heads.astype(jnp.float32))
    scores = scores * key_width ** (-0.5) * jnp.exp(exponent)
    weights_bf = scores.astype(jnp.bfloat16)
    inner_part = jnp.einsum('hts,shv->thv', weights_bf.astype(jnp.float32), value_head_rows.astype(jnp.float32))
    carried_portion = jnp.einsum('pix,ixe->pie', query_head_rows.astype(jnp.float32), carried_over, precision=lax.Precision.HIGHEST) * key_width ** (-0.5)
    carried_portion = carried_portion * jnp.transpose(jnp.exp(mstate[:, None] - run_max))[:, :, None]
    numerator = carried_portion + inner_part
    inv_rms = lax.rsqrt(lax.optimization_barrier(jnp.mean(numerator * numerator, axis=2, keepdims=True)) + EPS)
    gated_out = numerator * inv_rms * jax.nn.sigmoid(outgate.astype(jnp.float32).reshape(numerator.shape))
    return gated_out.reshape(length, -1).astype(jnp.bfloat16)

def advance(earlier, later_part):
    state_one_a, state_one_b, max_one, sum_one = earlier
    state_two_a, state_two_b, max_two, sum_two = later_part
    merged_max = jnp.maximum(sum_two + max_one, max_two)
    keep_old = jnp.exp(sum_two + max_one - merged_max)
    keep_new = jnp.exp(max_two - merged_max)
    merged_a = keep_old[0][:, None, None] * state_one_a + keep_new[0][:, None, None] * state_two_a
    merged_b = keep_old[1][:, None, None] * state_one_b + keep_new[1][:, None, None] * state_two_b
    return (merged_a, merged_b, merged_max, sum_one + sum_two)

def reference(query_a, key_a, query_b, key_b, values_a, values_b, outgate_a, outgate_b, input_pre, forget_pre, resid, out_proj, norm_gain, w_gate, w_up, w_down):
    block_count = SEQUENCE_LENGTH // TOK_DEV

    def blocks(array, width):
        return array.reshape(block_count, TOK_DEV, GROUP_HEADS, width)

    def gate_blocks(array):
        return jnp.transpose(array.reshape(2, GROUP_HEADS, block_count, TOK_DEV), (2, 0, 1, 3))
    inputs = (blocks(query_a, DKA), blocks(key_a, DKA), blocks(query_b, DKB), blocks(key_b, DKB), blocks(values_a, DV), blocks(values_b, DV), outgate_a.reshape(block_count, TOK_DEV, GROUP_HEADS * DV), outgate_b.reshape(block_count, TOK_DEV, GROUP_HEADS * DV), gate_blocks(input_pre), gate_blocks(forget_pre))

    def advance_block(carry_all, block_in):
        query_ha, key_ha, query_hb, key_hb, value_ha, value_hb, gate_oa, gate_ob, input_blk, forget_blk = block_in
        state_a, max_a, sum_a, offset_a = summarize(key_ha, value_ha, input_blk[0], forget_blk[0])
        state_b, max_b, sum_b, offset_b = summarize(key_hb, value_hb, input_blk[1], forget_blk[1])
        hidden_a = head_outputs(query_ha, key_ha, value_ha, gate_oa, offset_a, carry_all[0], carry_all[2][0], DKA)
        hidden_b = head_outputs(query_hb, key_hb, value_hb, gate_ob, offset_b, carry_all[1], carry_all[2][1], DKB)
        updated = advance(carry_all, (state_a, state_b, jnp.stack([max_a, max_b]), jnp.stack([sum_a, sum_b])))
        return (updated, jnp.stack([hidden_a, hidden_b], axis=1))
    initial = (jnp.zeros((GROUP_HEADS, DKA, DV), jnp.float32), jnp.zeros((GROUP_HEADS, DKB, DV), jnp.float32), jnp.full((2, GROUP_HEADS), NEG, jnp.float32), jnp.zeros((2, GROUP_HEADS), jnp.float32))
    unused, hidden = lax.scan(advance_block, initial, inputs)
    set_width = GROUP_HEADS // N_TP * DV
    hidden = hidden.reshape(SEQUENCE_LENGTH, 2, N_TP, set_width)
    proj_sets = out_proj.reshape(D, 2, N_TP, set_width)
    attn_out = jnp.zeros((SEQUENCE_LENGTH, D), jnp.float32)
    for member in range(N_TP):
        hidden_set = hidden[:, :, member, :].reshape(SEQUENCE_LENGTH, 2 * set_width)
        weight_set = proj_sets[:, :, member, :].reshape(D, 2 * set_width)
        partial_value = jnp.dot(hidden_set, jnp.transpose(weight_set), preferred_element_type=jnp.float32)
        attn_out = attn_out + lax.optimization_barrier(partial_value.astype(jnp.bfloat16)).astype(jnp.float32)
    resid_sum = resid.astype(jnp.float32) + attn_out
    normed = resid_sum * lax.rsqrt(lax.optimization_barrier(jnp.mean(resid_sum * resid_sum, axis=1, keepdims=True)) + EPS) * norm_gain
    normed = normed.astype(jnp.bfloat16)
    gate_act = jnp.dot(normed, w_gate, preferred_element_type=jnp.float32)
    up_act = jnp.dot(normed, w_up, preferred_element_type=jnp.float32)
    inner_act = (jax.nn.silu(gate_act) * up_act).astype(jnp.bfloat16)
    unit_width = FF // N_TP
    ffn_out = jnp.zeros((SEQUENCE_LENGTH, D), jnp.float32)
    for member in range(N_TP):
        inner_cols = inner_act[:, member * unit_width:(member + 1) * unit_width]
        down_cols = w_down[:, member * unit_width:(member + 1) * unit_width]
        partial_value = jnp.dot(inner_cols, jnp.transpose(down_cols), preferred_element_type=jnp.float32)
        ffn_out = ffn_out + lax.optimization_barrier(partial_value.astype(jnp.bfloat16)).astype(jnp.float32)
    return (resid_sum + ffn_out).astype(jnp.bfloat16)
```

```python
import jax
import jax.numpy as jnp
from jax import lax
from jax.sharding import PartitionSpec as P

DKA = 128
DKB = 64
DV = 256


EPS = 1e-06
NEG = -1e30


def summarize(key_heads, value_head_rows, input_log, forget_raw):
    cum_forget = jnp.cumsum(jax.nn.log_sigmoid(forget_raw), axis=1)
    offset_log = input_log - cum_forget
    block_sum = cum_forget[:, -1]
    block_max = block_sum + jnp.max(offset_log, axis=1)
    key_decay = jnp.exp(block_sum[:, None] + offset_log - block_max[:, None])
    scaled_keys = (key_heads.astype(jnp.float32) * jnp.transpose(key_decay)[:, :, None]).astype(
        jnp.bfloat16
    )
    block_memory_state = jnp.einsum(
        "eif,eiw->ifw", scaled_keys, value_head_rows, preferred_element_type=jnp.float32
    )
    return (block_memory_state, block_max, block_sum, offset_log)


def head_outputs(
    query_head_rows,
    key_heads,
    value_head_rows,
    outgate,
    offset_log,
    carried_over,
    mstate,
    key_width,
):
    length = query_head_rows.shape[0]
    run_max = jnp.maximum(lax.cummax(offset_log, axis=1), mstate[:, None])
    causal = jnp.arange(length)[:, None] >= jnp.arange(length)[None, :]
    exponent = jnp.where(causal[None], offset_log[:, None, :] - run_max[:, :, None], -jnp.inf)
    scores = jnp.einsum(
        "thk,shk->hts", query_head_rows, key_heads, preferred_element_type=jnp.float32
    )
    scores = scores * key_width ** (-0.5) * jnp.exp(exponent)
    weights_bf = scores.astype(jnp.bfloat16)
    inner_part = jnp.einsum(
        "hts,shv->thv", weights_bf, value_head_rows, preferred_element_type=jnp.float32
    )
    carried_portion = jnp.einsum(
        "pix,ixe->pie",
        query_head_rows,
        carried_over.astype(jnp.bfloat16),
        preferred_element_type=jnp.float32,
    ) * key_width ** (-0.5)
    carried_portion = (
        carried_portion * jnp.transpose(jnp.exp(mstate[:, None] - run_max))[:, :, None]
    )
    numerator = carried_portion + inner_part
    inv_rms = lax.rsqrt(jnp.mean(numerator * numerator, axis=2, keepdims=True) + EPS)
    gated_out = (
        numerator * inv_rms * jax.nn.sigmoid(outgate.astype(jnp.float32).reshape(numerator.shape))
    )
    return gated_out.reshape(length, -1).astype(jnp.bfloat16)


def shifted(value, axis, shift):
    count = lax.axis_size(axis)
    return lax.ppermute(value, axis, [(i, (i + shift) % count) for i in range(count)])


def swapped(value, axis):
    count = lax.axis_size(axis)
    return lax.ppermute(value, axis, [(i, i ^ 1) for i in range(count)])


def column_shifted(value, shift):
    count = lax.axis_size("tp")
    return lax.ppermute(value, "tp", [(i, (i + 2 * shift) % count) for i in range(count)])


def entering(states, stats):
    count, mine = lax.axis_size("sp"), lax.axis_index("sp")
    total = jnp.zeros_like(stats[1])
    highest = jnp.full_like(stats[0], NEG)
    logs, parts = [], []
    for step in range(1, count):
        pairs = [(i, i + step) for i in range(count - step)]
        stat = lax.ppermute(stats, "sp", pairs)
        parts.append([lax.ppermute(state, "sp", pairs) for state in states])
        log = jnp.where(step <= mine, stat[0] + total, NEG)
        total = total + stat[1]
        highest = jnp.maximum(highest, log)
        logs.append(log)
    carried = [jnp.zeros(state.shape, jnp.float32) for state in states]
    for step in range(1, count):
        weight = jnp.where(step <= mine, jnp.exp(logs[step - 1] - highest), 0.0)
        for group in range(2):
            carried[group] = carried[group] + weight[group][:, None, None] * parts[step - 1][
                group
            ].astype(jnp.float32)
    return carried, highest


def scatter_rows(partial):
    chips = lax.axis_size("tp") // 2
    me = lax.axis_index("tp")
    chip, core = me // 2, me % 2
    parts = partial.reshape(chips, 2, -1, partial.shape[-1])
    away = lax.dynamic_index_in_dim(parts, 1 - core, 1, keepdims=False).astype(jnp.bfloat16)
    kept = lax.dynamic_index_in_dim(parts, core, 1, keepdims=False)
    both = kept.astype(jnp.float32) + swapped(away, "tp").astype(jnp.float32)
    total = lax.dynamic_index_in_dim(both, chip, 0, keepdims=False)
    for step in range(1, chips):
        target = lax.rem(chip + step, chips)
        sent = lax.dynamic_index_in_dim(both, target, 0, keepdims=False).astype(jnp.bfloat16)
        total = total + column_shifted(sent, step).astype(jnp.float32)
    return total


def gather_rows(rows):
    chips = lax.axis_size("tp") // 2
    core = lax.axis_index("tp") % 2
    mine = jnp.stack([rows] + [column_shifted(rows, step) for step in range(1, chips)])
    other = swapped(mine, "tp")
    first = jnp.where(core == 0, mine, other)
    second = jnp.where(core == 0, other, mine)
    gathered = jnp.stack([first, second], axis=1)
    return gathered.reshape(-1, rows.shape[-1])


def by_owner(partial):
    chips = lax.axis_size("tp") // 2
    chip = lax.axis_index("tp") // 2
    parts = partial.reshape(chips, -1, partial.shape[-1])
    order = [
        lax.dynamic_index_in_dim(parts, lax.rem(chip - owner + chips, chips), 0)
        for owner in range(chips)
    ]
    return jnp.concatenate(order).reshape(partial.shape)


def local(
    query_a,
    key_a,
    query_b,
    key_b,
    values_a,
    values_b,
    outgate_a,
    outgate_b,
    input_pre,
    forget_pre,
    resid,
    out_proj,
    norm_gain,
    w_gate,
    w_up,
    w_down,
):
    tokens_dev = query_a.shape[0]
    heads_dev = query_a.shape[1] // DKA
    count, place, part = lax.axis_size("sp"), lax.axis_index("sp"), lax.axis_index("grp")
    depth, units = w_gate.shape
    half = units // 2
    side = lax.rem(place, 2)

    def columns(weight, step):
        target_side = lax.rem(place + step, 2)
        return lax.dynamic_slice_in_dim(weight, target_side * half, half, 1)

    lead = jnp.where(part == 0, w_gate, w_up)
    first_sent = columns(lead, 1)
    lead_parts = [None, shifted(first_sent, "sp", 1)]
    key_heads_a = key_a.reshape(tokens_dev, heads_dev, DKA)
    key_heads_b = key_b.reshape(tokens_dev, heads_dev, DKB)
    value_heads_a = values_a.reshape(tokens_dev, heads_dev, DV)
    value_heads_b = values_b.reshape(tokens_dev, heads_dev, DV)
    state_a, max_a, sum_a, offset_a = summarize(
        key_heads_a, value_heads_a, input_pre[0], forget_pre[0]
    )
    state_b, max_b, sum_b, offset_b = summarize(
        key_heads_b, value_heads_b, input_pre[1], forget_pre[1]
    )
    states = (state_a.astype(jnp.bfloat16), state_b.astype(jnp.bfloat16))
    stats = jnp.stack([jnp.stack([max_a, max_b]), jnp.stack([sum_a, sum_b])])
    lead, states, stats = lax.optimization_barrier((lead, states, stats))
    (carried_a, carried_b), mstate = entering(states, stats)
    for step in range(2, count):
        lead_parts.append(shifted(columns(lead, step), "sp", step))
    hidden_a = head_outputs(
        query_a.reshape(tokens_dev, heads_dev, DKA),
        key_heads_a,
        value_heads_a,
        outgate_a,
        offset_a,
        carried_a,
        mstate[0],
        DKA,
    )
    hidden_b = head_outputs(
        query_b.reshape(tokens_dev, heads_dev, DKB),
        key_heads_b,
        value_heads_b,
        outgate_b,
        offset_b,
        carried_b,
        mstate[1],
        DKB,
    )
    hidden = jnp.stack([hidden_a, hidden_b], axis=1).reshape(tokens_dev, -1)
    proj_weight = out_proj.reshape(out_proj.shape[0], -1)
    row_block = hidden
    attn_rows = scatter_rows(
        lax.dot_general(
            row_block, proj_weight, (((1,), (1,)), ((), ())), preferred_element_type=jnp.float32
        )
    )
    resid_sum = resid.astype(jnp.float32) + attn_rows
    normed = (
        resid_sum
        * lax.rsqrt(jnp.mean(resid_sum * resid_sum, axis=1, keepdims=True) + EPS)
        * norm_gain
    )
    normed = normed.astype(jnp.bfloat16)
    pair_normed = swapped(normed, "sp")
    w_down, normed = lax.optimization_barrier((w_down, normed))
    down_mine = lax.dynamic_slice_in_dim(w_down, part * (depth // 2), depth // 2, 0)
    down_parts = [None] + [
        shifted(columns(down_mine, step), "sp", step) for step in range(1, count)
    ]
    own = lambda weight: lax.dynamic_slice_in_dim(weight, side * half, half, 1)
    own_trail = jnp.where(part == 0, own(w_up), own(w_gate))
    lead_parts[0] = own(lead)
    trail_parts = [own_trail] + [swapped(piece, "grp") for piece in lead_parts[1:]]
    other_down = lax.dynamic_slice_in_dim(w_down, (1 - part) * (depth // 2), depth // 2, 0)
    down_parts[0] = own(down_mine)
    down_other = [own(other_down)] + [swapped(piece, "grp") for piece in down_parts[1:]]
    partials = []
    for rows in (gather_rows(normed), gather_rows(pair_normed)):
        lead_act = trail_act = 0.0
        for step in range(count):
            origin = lax.rem(place - step + count, count)
            block = lax.dynamic_slice_in_dim(rows, origin * depth, depth, 1)
            lead_act += jnp.dot(block, lead_parts[step], preferred_element_type=jnp.float32)
            trail_act += jnp.dot(block, trail_parts[step], preferred_element_type=jnp.float32)
        gate_act = jnp.where(part == 0, lead_act, trail_act)
        up_act = jnp.where(part == 0, trail_act, lead_act)
        inner_act = (jax.nn.silu(gate_act) * up_act).astype(jnp.bfloat16)
        pieces = []
        for step in range(count):
            for piece in (down_parts[step], down_other[step]):
                pieces.append(
                    lax.dot_general(
                        inner_act,
                        piece,
                        (((1,), (1,)), ((), ())),
                        preferred_element_type=jnp.float32,
                    ).astype(jnp.bfloat16)
                )
        summed = scatter_rows(by_owner(jnp.concatenate(pieces, axis=1)))
        blocks = summed.reshape(summed.shape[0], count, 2, depth // 2)
        blocks = jnp.where(part == 0, blocks, blocks[:, :, ::-1])
        ordered = [
            lax.dynamic_index_in_dim(blocks, lax.rem(place - owner + count, count), 1)
            for owner in range(count)
        ]
        partials.append(jnp.concatenate(ordered, axis=1).reshape(summed.shape))
    received = swapped(partials[1].astype(jnp.bfloat16), "sp").astype(jnp.float32)
    return (resid_sum + partials[0] + received).astype(jnp.bfloat16)


def solution(mesh):
    return jax.shard_map(
        local,
        mesh=mesh,
        in_specs=(
            P(("grp", "sp"), "tp"),
            P(("grp", "sp"), "tp"),
            P(("grp", "sp"), "tp"),
            P(("grp", "sp"), "tp"),
            P(("grp", "sp"), "tp"),
            P(("grp", "sp"), "tp"),
            P(("grp", "sp"), "tp"),
            P(("grp", "sp"), "tp"),
            P(None, "tp", ("grp", "sp")),
            P(None, "tp", ("grp", "sp")),
            P(("grp", "sp", "tp"), None),
            P(None, None, "tp"),
            P(),
            P("sp", "tp"),
            P("sp", "tp"),
            P("sp", "tp"),
        ),
        out_specs=P(("grp", "sp", "tp"), None),
        check_vma=False,
    )
```

```python
import jax
import jax.numpy as jnp
from jax import lax
from jax.sharding import PartitionSpec as P

DKA = 128
DKB = 64
DV = 256


EPS = 1e-06
NEG = -1e30


def summarize(key_heads, value_head_rows, input_log, forget_raw):
    cum_forget = jnp.cumsum(jax.nn.log_sigmoid(forget_raw), axis=1)
    offset_log = input_log - cum_forget
    block_sum = cum_forget[:, -1]
    block_max = block_sum + jnp.max(offset_log, axis=1)
    key_decay = jnp.exp(block_sum[:, None] + offset_log - block_max[:, None])
    scaled_keys = (key_heads.astype(jnp.float32) * jnp.transpose(key_decay)[:, :, None]).astype(
        jnp.bfloat16
    )
    block_memory_state = jnp.einsum(
        "eif,eiw->ifw", scaled_keys, value_head_rows, preferred_element_type=jnp.float32
    )
    return (block_memory_state, block_max, block_sum, offset_log)


def head_outputs(
    query_head_rows,
    key_heads,
    value_head_rows,
    outgate,
    offset_log,
    carried_over,
    mstate,
    key_width,
):
    length = query_head_rows.shape[0]
    run_max = jnp.maximum(lax.cummax(offset_log, axis=1), mstate[:, None])
    causal = jnp.arange(length)[:, None] >= jnp.arange(length)[None, :]
    exponent = jnp.where(causal[None], offset_log[:, None, :] - run_max[:, :, None], -jnp.inf)
    scores = jnp.einsum(
        "thk,shk->hts", query_head_rows, key_heads, preferred_element_type=jnp.float32
    )
    scores = scores * key_width ** (-0.5) * jnp.exp(exponent)
    weights_bf = scores.astype(jnp.bfloat16)
    inner_part = jnp.einsum(
        "hts,shv->thv", weights_bf, value_head_rows, preferred_element_type=jnp.float32
    )
    carried_portion = jnp.einsum(
        "pix,ixe->pie",
        query_head_rows,
        carried_over.astype(jnp.bfloat16),
        preferred_element_type=jnp.float32,
    ) * key_width ** (-0.5)
    carried_portion = (
        carried_portion * jnp.transpose(jnp.exp(mstate[:, None] - run_max))[:, :, None]
    )
    numerator = carried_portion + inner_part
    inv_rms = lax.rsqrt(jnp.mean(numerator * numerator, axis=2, keepdims=True) + EPS)
    gated_out = (
        numerator * inv_rms * jax.nn.sigmoid(outgate.astype(jnp.float32).reshape(numerator.shape))
    )
    return gated_out.reshape(length, -1).astype(jnp.bfloat16)


def shifted(value, axis, shift):
    count = lax.axis_size(axis)
    return lax.ppermute(value, axis, [(i, (i + shift) % count) for i in range(count)])


def swapped(value, axis):
    count = lax.axis_size(axis)
    return lax.ppermute(value, axis, [(i, i ^ 1) for i in range(count)])


def column_shifted(value, shift):
    count = lax.axis_size("tp")
    return lax.ppermute(value, "tp", [(i, (i + 2 * shift) % count) for i in range(count)])


def split_wide(value):
    high = lax.reduce_precision(value, 8, 7)
    middle = lax.reduce_precision(value - high, 8, 7)
    return jnp.stack([high, middle, value - high - middle]).astype(jnp.bfloat16)


def entering(state_a, state_b, stats):
    count, mine = lax.axis_size("sp"), lax.axis_index("sp")
    heads, depth_a, width = state_a.shape
    depth_b = state_b.shape[1]
    terms = split_wide(stats).transpose(3, 0, 1, 2).reshape(heads, 1, 12)
    terms = jnp.pad(terms, ((0, 0), (0, 15), (0, width - 12)))
    packed = jnp.concatenate(
        [state_a.astype(jnp.bfloat16), state_b.astype(jnp.bfloat16), terms], axis=1
    )
    parts = [
        lax.ppermute(packed, "sp", [(i, i + step) for i in range(count - step)])
        for step in range(1, count)
    ]
    total = jnp.zeros_like(stats[1])
    highest = jnp.full_like(stats[0], NEG)
    logs = []
    for step in range(1, count):
        got = parts[step - 1][:, depth_a + depth_b, :12].astype(jnp.float32)
        stat = jnp.sum(got.reshape(heads, 3, 2, 2), axis=1).transpose(1, 2, 0)
        logs.append(jnp.where(step <= mine, stat[0] + total, NEG))
        total = total + stat[1]
        highest = jnp.maximum(highest, logs[-1])
    carried_a, carried_b = jnp.zeros_like(state_a), jnp.zeros_like(state_b)
    for step in range(1, count):
        weight = jnp.where(step <= mine, jnp.exp(logs[step - 1] - highest), 0.0)[:, :, None, None]
        part = parts[step - 1].astype(jnp.float32)
        carried_a += weight[0] * part[:, :depth_a]
        carried_b += weight[1] * part[:, depth_a : depth_a + depth_b]
    return carried_a, carried_b, highest


def scatter_pair(partial):
    chips = lax.axis_size("tp") // 2
    me = lax.axis_index("tp")
    chip, core = me // 2, me % 2
    parts = partial.reshape(2, chips, 2, -1, partial.shape[-1])
    away = lax.dynamic_index_in_dim(parts, 1 - core, 2, keepdims=False).astype(jnp.bfloat16)
    kept = lax.dynamic_index_in_dim(parts, core, 2, keepdims=False)
    got = swapped(away, "tp")
    totals = []
    for which in (1, 0):
        both = kept[which].astype(jnp.float32) + got[which].astype(jnp.float32)
        total = lax.dynamic_index_in_dim(both, chip, 0, keepdims=False)
        for step in range(1, chips):
            target = lax.rem(chip + step, chips)
            sent = lax.dynamic_index_in_dim(both, target, 0, keepdims=False).astype(jnp.bfloat16)
            total = total + column_shifted(sent, step).astype(jnp.float32)
        totals.append(total)
    return totals[1] + swapped(totals[0].astype(jnp.bfloat16), "sp").astype(jnp.float32)


def scatter_rows(partial):
    chips = lax.axis_size("tp") // 2
    me = lax.axis_index("tp")
    chip, core = me // 2, me % 2
    parts = partial.reshape(chips, 2, -1, partial.shape[-1])
    away = lax.dynamic_index_in_dim(parts, 1 - core, 1, keepdims=False).astype(jnp.bfloat16)
    kept = lax.dynamic_index_in_dim(parts, core, 1, keepdims=False)
    both = kept.astype(jnp.float32) + swapped(away, "tp").astype(jnp.float32)
    total = lax.dynamic_index_in_dim(both, chip, 0, keepdims=False)
    for step in range(1, chips):
        target = lax.rem(chip + step, chips)
        sent = lax.dynamic_index_in_dim(both, target, 0, keepdims=False).astype(jnp.bfloat16)
        total = total + column_shifted(sent, step).astype(jnp.float32)
    return total


def gather_rows(rows):
    chips = lax.axis_size("tp") // 2
    core = lax.axis_index("tp") % 2
    mine = jnp.stack([rows] + [column_shifted(rows, step) for step in range(1, chips)])
    other = swapped(mine, "tp")
    first = jnp.where(core == 0, mine, other)
    second = jnp.where(core == 0, other, mine)
    gathered = jnp.stack([first, second], axis=1)
    return gathered.reshape(-1, rows.shape[-1])


def by_owner(partial):
    chips = lax.axis_size("tp") // 2
    chip = lax.axis_index("tp") // 2
    parts = partial.reshape(chips, -1, partial.shape[-1])
    order = [
        lax.dynamic_index_in_dim(parts, lax.rem(chip - owner + chips, chips), 0)
        for owner in range(chips)
    ]
    return jnp.concatenate(order).reshape(partial.shape)


def local(
    query_a,
    key_a,
    query_b,
    key_b,
    values_a,
    values_b,
    outgate_a,
    outgate_b,
    input_pre,
    forget_pre,
    resid,
    out_proj,
    norm_gain,
    w_gate,
    w_up,
    w_down,
):
    tokens_dev = query_a.shape[0]
    heads_dev = query_a.shape[1] // DKA
    count, place, part = lax.axis_size("sp"), lax.axis_index("sp"), lax.axis_index("grp")
    depth, units = w_gate.shape
    half = units // 2
    side = lax.rem(place, 2)

    def columns(weight, step):
        target_side = lax.rem(place + step, 2)
        return lax.dynamic_slice_in_dim(weight, target_side * half, half, 1)

    lead = jnp.where(part == 0, w_gate, w_up)
    first_sent = columns(lead, 1)
    lead_parts = [None, shifted(first_sent, "sp", 1)]
    key_heads_a = key_a.reshape(tokens_dev, heads_dev, DKA)
    key_heads_b = key_b.reshape(tokens_dev, heads_dev, DKB)
    value_heads_a = values_a.reshape(tokens_dev, heads_dev, DV)
    value_heads_b = values_b.reshape(tokens_dev, heads_dev, DV)
    state_a, max_a, sum_a, offset_a = summarize(
        key_heads_a, value_heads_a, input_pre[0], forget_pre[0]
    )
    state_b, max_b, sum_b, offset_b = summarize(
        key_heads_b, value_heads_b, input_pre[1], forget_pre[1]
    )
    stats = jnp.stack([jnp.stack([max_a, max_b]), jnp.stack([sum_a, sum_b])])
    lead, w_down, state_a, state_b, stats = lax.optimization_barrier(
        (lead, w_down, state_a, state_b, stats)
    )
    carried_a, carried_b, mstate = entering(state_a, state_b, stats)
    for step in range(2, count):
        lead_parts.append(shifted(columns(lead, step), "sp", step))
    down_mine = lax.dynamic_slice_in_dim(w_down, part * (depth // 2), depth // 2, 0)
    down_parts = [None] + [
        shifted(columns(down_mine, step), "sp", step) for step in range(1, count)
    ]
    hidden_a = head_outputs(
        query_a.reshape(tokens_dev, heads_dev, DKA),
        key_heads_a,
        value_heads_a,
        outgate_a,
        offset_a,
        carried_a,
        mstate[0],
        DKA,
    )
    hidden_b = head_outputs(
        query_b.reshape(tokens_dev, heads_dev, DKB),
        key_heads_b,
        value_heads_b,
        outgate_b,
        offset_b,
        carried_b,
        mstate[1],
        DKB,
    )
    hidden = jnp.stack([hidden_a, hidden_b], axis=1).reshape(tokens_dev, -1)
    proj_weight = out_proj.reshape(out_proj.shape[0], -1)
    row_block = hidden
    attn_rows = scatter_rows(
        lax.dot_general(
            row_block, proj_weight, (((1,), (1,)), ((), ())), preferred_element_type=jnp.float32
        )
    )
    resid_sum = resid.astype(jnp.float32) + attn_rows
    normed = (
        resid_sum
        * lax.rsqrt(jnp.mean(resid_sum * resid_sum, axis=1, keepdims=True) + EPS)
        * norm_gain
    )
    normed = normed.astype(jnp.bfloat16)
    pair_normed = swapped(normed, "sp")
    own = lambda weight: lax.dynamic_slice_in_dim(weight, side * half, half, 1)
    own_trail = jnp.where(part == 0, own(w_up), own(w_gate))
    lead_parts[0] = own(lead)
    trail_parts = [own_trail] + [swapped(piece, "grp") for piece in lead_parts[1:]]
    other_down = lax.dynamic_slice_in_dim(w_down, (1 - part) * (depth // 2), depth // 2, 0)
    down_parts[0] = own(down_mine)
    down_other = [own(other_down)] + [swapped(piece, "grp") for piece in down_parts[1:]]

    def placed(pieces, offset, blocks):
        whole = jnp.zeros((blocks * depth, half), jnp.bfloat16)
        for step, (first, second) in enumerate(pieces):
            origin = lax.rem(place - step + count, count) * depth
            whole = lax.dynamic_update_slice_in_dim(whole, first, origin + part * offset, 0)
            if second is not None:
                whole = lax.dynamic_update_slice_in_dim(
                    whole, second, origin + (1 - part) * offset, 0
                )
        return whole

    lead_full = placed([(piece, None) for piece in lead_parts], 0, count)
    trail_full = placed([(piece, None) for piece in trail_parts], 0, count)
    down_full = placed(list(zip(down_parts, down_other)), depth // 2, count)
    rows = jnp.concatenate([gather_rows(normed), gather_rows(pair_normed)])
    lead_act = jnp.dot(rows, lead_full, preferred_element_type=jnp.float32)
    trail_act = jnp.dot(rows, trail_full, preferred_element_type=jnp.float32)
    gate_act = jnp.where(part == 0, lead_act, trail_act)
    up_act = jnp.where(part == 0, trail_act, lead_act)
    inner_act = (jax.nn.silu(gate_act) * up_act).astype(jnp.bfloat16)
    partial = lax.dot_general(
        inner_act, down_full, (((1,), (1,)), ((), ())), preferred_element_type=jnp.float32
    ).astype(jnp.bfloat16)
    partial = partial.reshape(2, -1, partial.shape[-1])
    partial = jnp.stack([by_owner(partial[0]), by_owner(partial[1])])
    return (resid_sum + scatter_pair(partial)).astype(jnp.bfloat16)


def solution(mesh):
    return jax.shard_map(
        local,
        mesh=mesh,
        in_specs=(
            P(("grp", "sp"), "tp"),
            P(("grp", "sp"), "tp"),
            P(("grp", "sp"), "tp"),
            P(("grp", "sp"), "tp"),
            P(("grp", "sp"), "tp"),
            P(("grp", "sp"), "tp"),
            P(("grp", "sp"), "tp"),
            P(("grp", "sp"), "tp"),
            P(None, "tp", ("grp", "sp")),
            P(None, "tp", ("grp", "sp")),
            P(("grp", "sp", "tp"), None),
            P(None, None, "tp"),
            P(),
            P("sp", "tp"),
            P("sp", "tp"),
            P("sp", "tp"),
        ),
        out_specs=P(("grp", "sp", "tp"), None),
        check_vma=False,
    )
```
